768 devices in a mesh: rep: 3 (over z_hi), fs: 32 (over z_lo, y), tp: 8 (over x, core).
Axes of the slice: x: 4, y: 8, z: 12 (z_hi: 3, z_lo: 4; z = z_hi * 4 + z_lo), core: 2. Of those that a mesh axis runs over, the one named last changes fastest.
Arguments:
- tokens: bfloat16 [96, 512, 2048], P(('rep', 'fs')), may hold values from -6 to 6
- first_gain: float32 [2048], replicated, may hold values from 0.1 to 1.9
- in_matrix: float32 [2048, 2048], P('fs', 'tp'), may hold values from -0.125 to 0.125
- in_scale: float32 [2048], P('tp'), may hold values from 0.5 to 2
- conv_taps: float32 [4, 2048], P(None, 'tp'), may hold values from -3 to 3
- decay_rate: float32 [2, 2048], P(None, 'tp'), may hold values from 0 to 1, as said below
- recall_maps: float32 [2, 8, 256, 256], P(None, 'tp'), may hold values from -0.375 to 0.375
- admit_maps: float32 [2, 8, 256, 256], P(None, 'tp'), may hold values from -0.375 to 0.375
- out_matrix: float32 [2048, 2048], P('fs', 'tp'), may hold values from -0.125 to 0.125
- out_scale: float32 [2048], P('fs'), may hold values from 0.5 to 2
- second_gain: float32 [2048], replicated, may hold values from 0.1 to 1.9
- up_matrix: float32 [2048, 4096], P('fs', 'tp'), may hold values from -0.125 to 0.125
- up_scale: float32 [4096], P('tp'), may hold values from 0.5 to 2
- down_matrix: float32 [2048, 4096], P('fs', 'tp'), may hold values from -0.09375 to 0.09375
- down_scale: float32 [2048], P('fs'), may hold values from 0.5 to 2
Outputs:
- layer_out: bfloat16 [96, 512, 2048], P(('rep', 'fs'))
The draws below stay inside these ranges and needn't reach their ends.
Inputs may be any that keep to these rules, and one draw needn't show every extreme that they name: `decay_rate`: positive per-step decay rates.
All inputs are finite; a program needn't handle non-finite values.
Results may differ from the reference program's by a relative error of at most 0.024.
Values may be sent and summed in bfloat16 or wider, within the bound.
A program may use at most 64 MiB of HBM per device.

```python
import math
import jax
import jax.numpy as jnp
from jax import lax

D = 2048
BLOCK = 256
BLOCKS = 8
FF = 4096
TAPS = 4
LEN = 512
REC_WIDTH = 2048
SEQS = 96
N_TP = 8


def draw_decay_rate(key, part):
    pick_key, slow_key, fast_key = jax.random.split(jax.random.fold_in(key, 17), 3)
    shape = (2, REC_WIDTH)
    slow_share = 0.5
    slow_pick = jax.random.bernoulli(pick_key, slow_share, shape)
    slow_rate = jnp.exp(jax.random.uniform(slow_key, shape, jnp.float32, math.log(0.05), math.log(0.5))) / LEN
    fast_rate = jnp.exp(jax.random.uniform(fast_key, shape, jnp.float32, math.log(0.005), math.log(0.02)))
    return jnp.where(slow_pick, slow_rate, fast_rate).astype(jnp.float32)


def level_of(key, extent, cuts, least, top_value):
    factor_of, own = 1.0, jax.random.fold_in(key, 6)
    for dim, blocks in cuts:
        heights = jnp.exp(jax.random.uniform(jax.random.fold_in(own, dim), (blocks,), jnp.float32, least / len(cuts), top_value / len(cuts)))
        factor_of = factor_of * jnp.repeat(heights, extent[dim] // blocks).reshape([-1 if axis == dim else 1 for axis in range(len(extent))])
    return factor_of


def bell_draw(rng, dims, deviation, reach, pieces=(), dtype=jnp.bfloat16):
    level = level_of(rng, dims, pieces, -0.22, 0.18) if pieces else 1.0
    entries = jax.random.normal(rng, dims, jnp.float32) * deviation * level
    return jnp.minimum(jnp.maximum(entries, -reach), reach).astype(dtype)


def setup_inputs(seed: int = 0) -> dict:
    seeds = jax.random.split(jax.random.key(seed), 16)
    return {
        "tokens": bell_draw(seeds[0], (SEQS, LEN, D), 1.0, 6.0, ((0, 96),)),
        "first_gain": jnp.clip(1.0 + 0.18 * jax.random.normal(seeds[1], (D,), jnp.float32), 0.1, 1.9),
        "in_matrix": bell_draw(seeds[2], (D, REC_WIDTH), D ** -0.5, 0.125, ((0, 32), (1, 8)), jnp.float32),
        "in_scale": jnp.clip(jnp.exp(math.log(2.0) - 1.3862944 * jax.random.uniform(seeds[3], (REC_WIDTH,), jnp.float32) ** level_of(seeds[3], (REC_WIDTH,), ((0, 8),), -0.2, 0.2)), 0.5, 2.0),
        "conv_taps": bell_draw(seeds[4], (TAPS, REC_WIDTH), TAPS ** -0.5, 3.0, ((1, 8),), jnp.float32),
        "decay_rate": draw_decay_rate(jax.random.fold_in(seeds[15], 71), 0),
        "recall_maps": bell_draw(seeds[6], (2, BLOCKS, BLOCK, BLOCK), BLOCK ** -0.5, 0.375, ((1, 8),), jnp.float32),
        "admit_maps": bell_draw(seeds[7], (2, BLOCKS, BLOCK, BLOCK), BLOCK ** -0.5, 0.375, ((1, 8),), jnp.float32),
        "out_matrix": bell_draw(seeds[8], (D, REC_WIDTH), REC_WIDTH ** -0.5, 0.125, ((0, 32), (1, 8)), jnp.float32),
        "out_scale": jnp.clip(jnp.exp(math.log(2.0) - 1.3862944 * jax.random.uniform(seeds[9], (D,), jnp.float32) ** level_of(seeds[9], (D,), ((0, 32),), -0.2, 0.2)), 0.5, 2.0),
        "second_gain": jnp.clip(1.0 + 0.18 * jax.random.normal(seeds[10], (D,), jnp.float32), 0.1, 1.9),
        "up_matrix": bell_draw(seeds[11], (D, FF), D ** -0.5, 0.125, ((0, 32), (1, 8)), jnp.float32),
        "up_scale": jnp.clip(jnp.exp(math.log(2.0) - 1.3862944 * jax.random.uniform(seeds[12], (FF,), jnp.float32) ** level_of(seeds[12], (FF,), ((0, 8),), -0.2, 0.2)), 0.5, 2.0),
        "down_matrix": bell_draw(seeds[13], (D, FF), FF ** -0.5, 0.09375, ((0, 32), (1, 8)), jnp.float32),
        "down_scale": jnp.clip(jnp.exp(math.log(2.0) - 1.3862944 * jax.random.uniform(seeds[14], (D,), jnp.float32) ** level_of(seeds[14], (D,), ((0, 32),), -0.2, 0.2)), 0.5, 2.0),
    }


EPSILON = 1e-06
RATE_GAIN = 8.0

def normalize(stream, gain):
    return stream * lax.rsqrt(lax.optimization_barrier(jnp.mean(stream * stream, axis=-1, keepdims=True)) + EPSILON) * gain

def convolve(values, taps):
    length = values.shape[0]
    count = taps.shape[0]
    padded = jnp.pad(values, ((count // 2, count - 1 - count // 2), (0, 0)))
    total = taps[0] * padded[0:length]
    for offset in range(1, count):
        total = total + taps[offset] * padded[offset:offset + length]
    return total

def block_map(values, maps):
    length = values.shape[0]
    count, width = (maps.shape[0], maps.shape[1])
    grouped = values.reshape(length, count, width)
    mapped = jnp.einsum('lnj,njk->lnk', grouped, maps, precision=lax.Precision.HIGHEST)
    return mapped.reshape(length, count * width)

def combine_steps(earlier, later):
    return (earlier[0] * later[0], later[0] * earlier[1] + later[1])

def one_direction(values, rate, recall_map, admit_map):
    recall = jax.nn.sigmoid(block_map(values, recall_map))
    admit = jax.nn.sigmoid(block_map(values, admit_map))
    log_decay = -RATE_GAIN * recall * rate
    decay = jnp.exp(log_decay)
    drive = jnp.sqrt(-jnp.expm1(2.0 * log_decay)) * admit * values
    carried = lax.associative_scan(combine_steps, (decay, drive), axis=0)
    return carried[1]

def recurrence(values, rates, recall_maps, admit_maps):
    forward = one_direction(values, rates[0], recall_maps[0], admit_maps[0])
    backward = one_direction(values[::-1], rates[1], recall_maps[1], admit_maps[1])[::-1]
    return forward + backward

def block_sum(values, matrix):
    length, width = values.shape
    model = matrix.shape[0]
    split_values = values.astype(jnp.float32).reshape(length, N_TP, width // N_TP)
    split_matrix = matrix.astype(jnp.float32).reshape(model, N_TP, width // N_TP)
    parts = jnp.einsum('lte,dte->tld', split_values, split_matrix, precision=lax.Precision.HIGHEST)
    rounded = lax.optimization_barrier(parts.astype(jnp.bfloat16))
    return lax.optimization_barrier(jnp.sum(rounded.astype(jnp.float32), axis=0))

def reference(tokens, first_gain, in_matrix, in_scale, conv_taps, decay_rate, recall_maps, admit_maps, out_matrix, out_scale, second_gain, up_matrix, up_scale, down_matrix, down_scale):
    in_cols = in_matrix.astype(jnp.bfloat16)
    out_rows = out_matrix.astype(jnp.bfloat16)
    up_cols = up_matrix.astype(jnp.bfloat16)
    down_rows = down_matrix.astype(jnp.bfloat16)
    in_factor = in_scale.astype(jnp.bfloat16)
    out_factor = out_scale.astype(jnp.bfloat16)
    up_factor = up_scale.astype(jnp.bfloat16)
    down_factor = down_scale.astype(jnp.bfloat16)

    def one_sequence(sequence):
        stream = sequence.astype(jnp.float32)
        normed = normalize(stream, first_gain).astype(jnp.bfloat16)
        before = (jnp.dot(normed, in_cols, preferred_element_type=jnp.float32) * in_factor).astype(jnp.bfloat16)
        conv_out = convolve(before.astype(jnp.float32), conv_taps)
        mixed = recurrence(conv_out, decay_rate, recall_maps, admit_maps).astype(jnp.bfloat16)
        middle = stream + out_factor * block_sum(mixed, out_rows)
        second_normed = normalize(middle, second_gain).astype(jnp.bfloat16)
        raised = jnp.dot(second_normed, up_cols, preferred_element_type=jnp.float32) * up_factor
        active = jnp.square(jax.nn.relu(raised)).astype(jnp.bfloat16)
        return (middle + down_factor * block_sum(active, down_rows)).astype(jnp.bfloat16)
    return lax.map(one_sequence, tokens)
```

```python
import functools

import jax
import jax.numpy as jnp
from jax import lax
from jax.experimental import pallas as pl
from jax.experimental.pallas import tpu as pltpu
from jax.sharding import PartitionSpec as P

EPSILON = 1e-06
RATE_GAIN = 8.0
MESH = pl.DeviceIdType.MESH
F32, BF16 = jnp.float32, jnp.bfloat16
NZ, NY, NX = 4, 8, 4
CHUNK, CHUNKS = 64, 8
PAD = 8
COPIES = 120


def nt_dot(left, right):
    return lax.dot_general(left, right, (((1,), (1,)), ((), ())), preferred_element_type=F32)


def as_column(row):
    n = row.shape[1]
    eye = lax.broadcasted_iota(jnp.int32, (n, n), 0) == lax.broadcasted_iota(jnp.int32, (n, n), 1)
    return jnp.sum(jnp.where(eye, jnp.broadcast_to(row, (n, n)), 0.0), axis=1, keepdims=True)


def rounded(value):
    return value.astype(BF16).astype(F32)


def kernel(
    tokens, first_gain, in_matrix, in_scale, conv_taps, decay_rate, recall_maps, admit_maps,
    out_matrix, out_scale, second_gain, up_matrix, up_scale, down_matrix, down_scale,
    result,
    in_all, out_all, up_all, down_all, normed, padded, conv, recall, admit, state, gain, mixed,
    part, paired, sums, relay_a, relay_b, from_left, from_right, middle, second, active,
    part2, paired2, sums2, relay2_a, relay2_b, from_left2, from_right2,
    send_sem, recv_sem,
):
    r, f, t = lax.axis_index("rep"), lax.axis_index("fs"), lax.axis_index("tp")
    zl, y = f // NY, f % NY
    z, depth = r * NZ + zl, 3 * NZ
    x, c = t // 2, t % 2
    z_up, z_down = (z + 1) % depth, (z + depth - 1) % depth
    Y_UP, Y_DOWN = (r, zl * NY + (y + 1) % NY, t), (r, zl * NY + (y + NY - 1) % NY, t)
    Z_UP, Z_DOWN = (z_up // NZ, (z_up % NZ) * NY + y, t), (z_down // NZ, (z_down % NZ) * NY + y, t)
    X_UP, X_DOWN = (r, f, (t + 2) % 8), (r, f, (t + 6) % 8)
    TWIN = (r, f, t + 1 - 2 * c)

    barrier = pltpu.get_barrier_semaphore()
    for peer in (Y_UP, Y_DOWN, Z_UP, Z_DOWN, X_UP, X_DOWN, TWIN):
        pl.semaphore_signal(barrier, inc=1, device_id=peer, device_id_type=MESH)

    started = []

    def send(src, dst, peer):
        k = len(started)
        copy = pltpu.make_async_remote_copy(
            src_ref=src, dst_ref=dst, send_sem=send_sem.at[k], recv_sem=recv_sem.at[k],
            device_id=peer, device_id_type=MESH,
        )
        copy.start()
        started.append(copy)
        return copy

    class Gather:
        def __init__(self, buf, split):
            self.buf, self.split, self.rows, self.waiting = buf, split, buf.shape[2], []
            self.step = 0

        def both(self, up, src_up, down, src_down):
            self.waiting.append(send(src_up, src_up, up))
            self.waiting.append(send(src_down, src_down, down))

        def go(self):
            for copy in self.waiting:
                copy.wait_recv()
            self.waiting = []
            buf, k = self.buf, self.step
            self.step += 1
            if self.split > 0:
                lo, mid, hi = 0, self.split // 2, self.split
                if k == 0:
                    own = buf.at[zl, y, lo:hi]
                    self.both(Z_UP, own, Z_DOWN, own)
                elif k == 1:
                    self.both(Z_UP, buf.at[(zl + 3) % NZ, y, lo:mid], Z_DOWN, buf.at[(zl + 1) % NZ, y, mid:hi])
                elif k in (2, 3, 4):
                    d = k - 2
                    self.both(Y_UP, buf.at[:, (y + NY - d) % NY, lo:hi], Y_DOWN, buf.at[:, (y + d) % NY, lo:hi])
                elif k == 5:
                    self.both(Y_UP, buf.at[:, (y + NY - 3) % NY, lo:mid], Y_DOWN, buf.at[:, (y + 3) % NY, mid:hi])
            if self.split < self.rows:
                lo, hi = self.split, self.rows
                mid = (lo + hi) // 2
                if k in (0, 1, 2):
                    self.both(Y_UP, buf.at[zl, (y + NY - k) % NY, lo:hi], Y_DOWN, buf.at[zl, (y + k) % NY, lo:hi])
                elif k == 3:
                    self.both(Y_UP, buf.at[zl, (y + NY - 3) % NY, lo:mid], Y_DOWN, buf.at[zl, (y + 3) % NY, mid:hi])
                elif k == 4:
                    own = buf.at[zl, :, lo:hi]
                    self.both(Z_UP, own, Z_DOWN, own)
                elif k == 5:
                    self.both(Z_UP, buf.at[(zl + 3) % NZ, :, lo:mid], Z_DOWN, buf.at[(zl + 1) % NZ, :, mid:hi])

    in_all[zl, y] = in_matrix[...].astype(BF16)
    out_all[zl, y] = (rounded(out_matrix[...]) * as_column(rounded(out_scale[...]))).astype(BF16)
    pl.semaphore_wait(barrier, 7)
    g_in, g_out = Gather(in_all, 32), Gather(out_all, 32)
    g_up, g_down = Gather(up_all, 64), Gather(down_all, 0)
    g_in.go()
    g_out.go()
    up_all[zl, y] = up_matrix[...].astype(BF16)
    down_all[zl, y] = (rounded(down_matrix[...]) * as_column(rounded(down_scale[...]))).astype(BF16)

    def normalize_rows(first, count):
        def step(i, carry):
            rows = pl.ds(pl.multiple_of(first + i * 32, 32), 32)
            value = tokens[0, rows, :].astype(F32)
            scale = lax.rsqrt(jnp.mean(value * value, axis=-1, keepdims=True) + EPSILON)
            normed[rows, :] = (value * scale * first_gain[...]).astype(BF16)
            return carry

        lax.fori_loop(0, count // 32, step, 0)

    for k in range(4):
        normalize_rows(128 * k, 128)
        g_in.go()
        g_out.go()
    padded[:, 0:PAD, :] = jnp.zeros((2, PAD, 128), F32)
    padded[:, PAD + 512 :, :] = jnp.zeros((2, PAD, 128), F32)
    g_in.go()
    g_out.go()
    g_in.go()
    g_out.go()
    g_down.go()
    g_up.go()

    def project(i, carry):
        rows = pl.ds(pl.multiple_of(i * 256, 256), 256)
        value = jnp.dot(normed[rows, :], in_all[...].reshape(2048, 256), preferred_element_type=F32)
        value = rounded(value * rounded(in_scale[...]))
        there = pl.ds(pl.multiple_of(PAD + i * 256, 8), 256)
        padded[0, there, :] = value[:, 0:128]
        padded[1, there, :] = value[:, 128:256]
        return carry

    lax.fori_loop(0, 2, project, 0)
    g_down.go()
    g_up.go()

    for half in range(2):
        lanes = pl.ds(half * 128, 128)
        taps = [conv_taps[k : k + 1, half * 128 : half * 128 + 128] for k in range(4)]

        def convolve(i, window):
            ahead = padded[half, pl.ds(i + PAD + 1, CHUNKS, stride=CHUNK), :]
            window = (*window, ahead)
            total = taps[0] * window[0] + taps[1] * window[1] + taps[2] * window[2] + taps[3] * window[3]
            conv[pl.ds(pl.multiple_of(i * 8, 8), 8), lanes] = total
            return window[1:]

        head = tuple(padded[half, pl.ds(PAD - 2 + k, CHUNKS, stride=CHUNK), :] for k in range(3))
        lax.fori_loop(0, CHUNK, convolve, head, unroll=4)

    g_down.go()
    g_up.go()
    values = conv[...].astype(BF16)
    for d in range(2):
        recall[d] = jnp.dot(values, recall_maps[d, 0].astype(BF16), preferred_element_type=F32)
        admit[d] = jnp.dot(values, admit_maps[d, 0].astype(BF16), preferred_element_type=F32)
    g_down.go()
    g_up.go()

    rates = [decay_rate[d : d + 1, :] * RATE_GAIN for d in range(2)]

    def scan_step(i, carry):
        new = []
        for d in range(2):
            h, g = carry[2 * d], carry[2 * d + 1]
            at = i if d == 0 else CHUNK - 1 - i
            rows = pl.ds(pl.multiple_of(at * 8, 8), 8)
            rate = 1.0 / (1.0 + jnp.exp(-recall[d, rows, :])) * rates[d]
            a = jnp.exp(-rate)
            u = jnp.tanh(rate)
            root = 2.0 * u * lax.rsqrt(jnp.maximum(2.0 * u * (1.0 + u), 1e-37))
            drive = root / (1.0 + jnp.exp(-admit[d, rows, :])) * conv[rows, :]
            h = a * h + drive
            g = a * g
            state[d, rows, :] = h
            gain[d, rows, :] = g
            new += [h, g]
        return tuple(new)

    zero, one = jnp.zeros((CHUNKS, 256), F32), jnp.ones((CHUNKS, 256), F32)
    ends = lax.fori_loop(0, CHUNK, scan_step, (zero, one, zero, one), unroll=4)

    def carried(h, g, order):
        row, rows = jnp.zeros((1, 256), F32), {}
        for s in order:
            rows[s] = row
            row = g[s : s + 1, :] * row + h[s : s + 1, :]
        return jnp.concatenate([rows[s] for s in range(CHUNKS)], axis=0)

    carry_0 = carried(ends[0], ends[1], range(CHUNKS))
    carry_1 = carried(ends[2], ends[3], range(CHUNKS - 1, -1, -1))

    def finish(i, carry):
        rows = pl.ds(pl.multiple_of(i * 8, 8), 8)
        total = state[0, rows, :] + gain[0, rows, :] * carry_0 + (state[1, rows, :] + gain[1, rows, :] * carry_1)
        mixed[0, pl.ds(i, CHUNKS, stride=CHUNK), :] = total[:, 0:128]
        mixed[1, pl.ds(i, CHUNKS, stride=CHUNK), :] = total[:, 128:256]
        return carry

    lax.fori_loop(0, CHUNK, finish, 0, unroll=4)
    g_down.go()
    g_up.go()

    x1, x2, x3 = (x + 1) % NX, (x + 2) % NX, (x + 3) % NX

    def summed_at_owner(left, weight, part, paired, sums, relay_a, relay_b, from_left, from_right, between):
        def tile(n, carry):
            w = weight[n // 2, pl.ds((n % 2) * 4, 4)]
            value = nt_dot(left, w.reshape(256, w.shape[-1])).astype(BF16)
            part[:, :, :, pl.ds(pl.multiple_of(n * 256, 256), 256)] = value.reshape(4, 2, 64, 256)
            return carry

        cols = (slice(0, 1024), slice(1024, 2048))
        twin = []
        for half in range(2):
            lax.fori_loop(4 * half, 4 * half + 4, tile, 0)
            twin.append(send(part.at[:, 1 - c, :, cols[half]], paired.at[:, :, cols[half]], TWIN))

        def pair_sum(owner, half):
            return part[owner, c, :, cols[half]].astype(F32) + paired[owner, :, cols[half]].astype(F32)

        twin[0].wait_recv()
        sums[2, :, cols[0]] = pair_sum(x2, 0).astype(BF16)
        relayed_a = send(sums.at[2, :, cols[0]], relay_a, X_DOWN)
        sums[1, :, cols[0]] = pair_sum(x1, 0).astype(BF16)
        left_a = send(sums.at[1, :, cols[0]], from_left.at[:, cols[0]], X_UP)
        twin[1].wait_recv()
        sums[2, :, cols[1]] = pair_sum(x2, 1).astype(BF16)
        relayed_b = send(sums.at[2, :, cols[1]], relay_b, X_UP)
        sums[3, :, cols[1]] = pair_sum(x3, 1).astype(BF16)
        right_b = send(sums.at[3, :, cols[1]], from_right.at[:, cols[1]], X_DOWN)
        relayed_a.wait_recv()
        sums[3, :, cols[0]] = (pair_sum(x3, 0) + relay_a[...].astype(F32)).astype(BF16)
        right_a = send(sums.at[3, :, cols[0]], from_right.at[:, cols[0]], X_DOWN)
        relayed_b.wait_recv()
        sums[1, :, cols[1]] = (pair_sum(x1, 1) + relay_b[...].astype(F32)).astype(BF16)
        left_b = send(sums.at[1, :, cols[1]], from_left.at[:, cols[1]], X_UP)
        between()
        for copy in (left_a, right_b, right_a, left_b):
            copy.wait_recv()
        own = part[x, c].astype(F32) + paired[x].astype(F32)
        return own + from_left[...].astype(F32) + from_right[...].astype(F32)

    def to_everyone(block):
        half_a, half_b = slice(0, 1024), slice(1024, 2048)
        below, above, across = (t + 6) % 8, (t + 2) % 8, (t + 4) % 8
        up = send(block(t), block(t), X_UP)
        down = send(block(t), block(t), X_DOWN)
        last = [send(block(t), block(t), TWIN)]
        up.wait_recv()
        over_a = send(block(below).at[:, half_a], block(below).at[:, half_a], X_UP)
        last.append(send(block(below), block(below), TWIN))
        down.wait_recv()
        over_b = send(block(above).at[:, half_b], block(above).at[:, half_b], X_DOWN)
        last.append(send(block(above), block(above), TWIN))
        over_a.wait_recv()
        last.append(send(block(across).at[:, half_a], block(across).at[:, half_a], TWIN))
        over_b.wait_recv()
        last.append(send(block(across).at[:, half_b], block(across).at[:, half_b], TWIN))
        for copy in last:
            copy.wait_recv()

    def more_weights():
        g_down.go()
        g_up.go()

    own_rows = pl.ds(pl.multiple_of(t * 64, 64), 64)
    mixed_b = jnp.concatenate([mixed[0], mixed[1]], axis=1).astype(BF16)
    mix = summed_at_owner(
        mixed_b, out_all, part, paired, sums, relay_a, relay_b, from_left, from_right, more_weights
    )
    value = tokens[0, own_rows, :].astype(F32) + mix
    middle[...] = value
    scale = lax.rsqrt(jnp.mean(value * value, axis=-1, keepdims=True) + EPSILON)
    second[t] = (value * scale * second_gain[...]).astype(BF16)
    to_everyone(lambda b: second.at[b])
    more_weights()

    def raise_rows(i, carry):
        rows = pl.ds(i * 4, 4)
        left = second[rows].reshape(256, 2048)
        for n in range(2):
            cols = slice(n * 256, n * 256 + 256)
            value = jnp.dot(left, up_all[:, :, :, cols].reshape(2048, 256), preferred_element_type=F32)
            value = jnp.maximum(value * rounded(up_scale[:, cols]), 0.0)
            active[pl.ds(pl.multiple_of(i * 256, 256), 256), cols] = (value * value).astype(BF16)
        return carry

    lax.fori_loop(0, 2, raise_rows, 0)
    down = summed_at_owner(
        active[...], down_all, part2, paired2, sums2, relay2_a, relay2_b, from_left2, from_right2, lambda: None
    )
    result[t] = (middle[...] + down).astype(BF16)
    to_everyone(lambda b: result.at[b])
    for copy in started:
        copy.wait_send()


def body(
    tokens, first_gain, in_matrix, in_scale, conv_taps, decay_rate, recall_maps, admit_maps,
    out_matrix, out_scale, second_gain, up_matrix, up_scale, down_matrix, down_scale,
):
    row = lambda v: v.reshape(1, -1)
    vmem = pl.BlockSpec(memory_space=pltpu.VMEM)
    ring = [
        pltpu.VMEM((4, 2, 64, 2048), BF16),
        pltpu.VMEM((4, 64, 2048), BF16),
        pltpu.VMEM((4, 64, 2048), BF16),
        pltpu.VMEM((64, 1024), BF16),
        pltpu.VMEM((64, 1024), BF16),
        pltpu.VMEM((64, 2048), BF16),
        pltpu.VMEM((64, 2048), BF16),
    ]
    out = pl.pallas_call(
        kernel,
        out_shape=jax.ShapeDtypeStruct((8, 64, 2048), BF16),
        in_specs=[vmem] * 15,
        out_specs=vmem,
        scratch_shapes=[
            pltpu.VMEM((NZ, NY, 64, 256), BF16),
            pltpu.VMEM((NZ, NY, 64, 256), BF16),
            pltpu.VMEM((NZ, NY, 64, 512), BF16),
            pltpu.VMEM((NZ, NY, 64, 512), BF16),
            pltpu.VMEM((512, 2048), BF16),
            pltpu.VMEM((2, 512 + 2 * PAD, 128), F32),
            pltpu.VMEM((512, 256), F32),
            pltpu.VMEM((2, 512, 256), F32),
            pltpu.VMEM((2, 512, 256), F32),
            pltpu.VMEM((2, 512, 256), F32),
            pltpu.VMEM((2, 512, 256), F32),
            pltpu.VMEM((2, 512, 128), F32),
            *ring,
            pltpu.VMEM((64, 2048), F32),
            pltpu.VMEM((8, 64, 2048), BF16),
            pltpu.VMEM((512, 512), BF16),
            *ring,
            pltpu.SemaphoreType.DMA((COPIES,)),
            pltpu.SemaphoreType.DMA((COPIES,)),
        ],
        compiler_params=pltpu.CompilerParams(
            collective_id=0, has_side_effects=True, vmem_limit_bytes=60 * 1024 * 1024
        ),
        name="layer",
    )(
        tokens, row(first_gain), in_matrix, row(in_scale), conv_taps, decay_rate, recall_maps, admit_maps,
        out_matrix, row(out_scale), row(second_gain), up_matrix, row(up_scale), down_matrix, row(down_scale),
    )
    return out.reshape(tokens.shape)


def solution(mesh):
    placed = (
        P(("rep", "fs"), None, None),
        P(),
        P("fs", "tp"),
        P("tp"),
        P(None, "tp"),
        P(None, "tp"),
        P(None, "tp", None, None),
        P(None, "tp", None, None),
        P("fs", "tp"),
        P("fs"),
        P(),
        P("fs", "tp"),
        P("tp"),
        P("fs", "tp"),
        P("fs"),
    )
    return jax.shard_map(
        body, mesh=mesh, in_specs=placed, out_specs=P(("rep", "fs"), None, None), check_vma=False
    )
```
